32 devices in a mesh: grp: 2 (over y), sp: 4 (over z), tp: 4 (over x, core).
Axes of the slice: x: 2, y: 2, z: 4, core: 2. Of those that a mesh axis runs over, the one named last changes fastest.
Arguments:
- stream: bfloat16 [4096, 2048], P(('grp', 'sp')), parts along dimension 0, may hold values from -6 to 6
- queries_a: bfloat16 [4096, 512], P(('grp', 'sp'), 'tp'), parts along dimension 0, may hold values from -6 to 6
- keys_a: bfloat16 [4096, 512], P(('grp', 'sp'), 'tp'), parts along dimension 0, may hold values from -6 to 6
- queries_b: bfloat16 [4096, 1024], P(('grp', 'sp'), 'tp'), parts along dimension 0, may hold values from -6 to 6
- keys_b: bfloat16 [4096, 1024], P(('grp', 'sp'), 'tp'), parts along dimension 0, may hold values from -6 to 6
- values: bfloat16 [4096, 2, 1024], P(('grp', 'sp'), None, 'tp'), parts along dimension 0, may hold values from -6 to 6
- out_gate: bfloat16 [4096, 2, 1024], P(('grp', 'sp'), None, 'tp'), parts along dimension 0, may hold values from -6 to 6
- in_gate: float32 [2, 8, 4096], P(None, 'tp', ('grp', 'sp')), parts along dimension 2, may hold values from -4 to 250
- forget_gate: float32 [2, 8, 4096], P(None, 'tp', ('grp', 'sp')), parts along dimension 2, may hold values from -5 to 16
- head_gain: float32 [2, 1024], P(None, 'tp'), may hold values from 0.1 to 1.9
- out_weight: bfloat16 [2, 1024, 2048], P(None, 'tp'), may hold values from -0.125 to 0.125
- norm_gain: float32 [2048], replicated, may hold values from 0.1 to 1.9
- gate_weight: bfloat16 [2048, 5632], P('sp', 'tp'), may hold values from -0.125 to 0.125
- up_weight: bfloat16 [2048, 5632], P('sp', 'tp'), may hold values from -0.125 to 0.125
- down_weight: bfloat16 [5632, 2048], P('tp', 'sp'), may hold values from -0.078125 to 0.078125
Outputs:
- layer_out: bfloat16 [4096, 2048], P(('grp', 'sp', 'tp')), parts along dimension 0
The draws below stay inside these ranges and needn't reach their ends.
There are 2 independent parts, one for each index of `grp`. The reference program is written for one: setup_inputs(seed, part) draws one part's arguments, and reference() takes and returns one part's arrays. A program takes and returns all parts, laid end to end along the dimension named above; an argument that names none is the same for every part. Nothing has to cross between parts.
All inputs are finite; a program needn't handle non-finite values.
Results may differ from the reference program's by a relative error of at most 0.013.
Values may be sent and summed in bfloat16 or wider, within the bound.
A program may use at most 128 MiB of HBM per device.

```python
import math
import jax
import jax.numpy as jnp
from jax import lax

D = 2048
HALF = 8
DKA = 64
DKB = 128
DV = 128
FF = 5632
TOK_DEV = 512
SEQUENCE_TOKENS = 2048
N_TP = 4


def draw_forget_gate(key, part):
    key_rows = jax.random.split(jax.random.fold_in(key, 17), 7)
    tensor_dims = (2, HALF, SEQUENCE_TOKENS)
    slow_share = 0.5
    slow = jax.random.uniform(key_rows[0], (2, HALF, 1)) < slow_share
    slow_rate = jnp.exp(jax.random.uniform(key_rows[1], (2, HALF, 1), minval=math.log(0.1), maxval=math.log(0.4))) / SEQUENCE_TOKENS
    span = jnp.exp(jax.random.uniform(key_rows[2], (2, HALF, 1), minval=math.log(max(TOK_DEV / 16, 2.0)), maxval=math.log(max(TOK_DEV / 5, 4.0))))
    rate = jnp.where(slow, slow_rate, 1.0 / span)
    factor = jnp.exp(jax.random.uniform(key_rows[3], (2, HALF, SEQUENCE_TOKENS // TOK_DEV), minval=0.0, maxval=math.log(4.0)))
    rate = rate * jnp.repeat(factor, TOK_DEV, axis=2)
    noise = jnp.clip(0.7 * jax.random.normal(key_rows[4], tensor_dims), -2.5, 2.5)
    preactivation = -jnp.log(jnp.expm1(rate)) + noise
    gate_spike = jax.random.uniform(key_rows[5], tensor_dims) < 3.0 / SEQUENCE_TOKENS
    retained_rows = jax.random.uniform(key_rows[6], tensor_dims, minval=0.5, maxval=0.8)
    return jnp.where(gate_spike, jnp.log(retained_rows / (1.0 - retained_rows)), preactivation).astype(jnp.float32)


def draw_in_gate(key, part):
    key_rows = jax.random.split(jax.random.fold_in(key, 23), 1)
    tensor_dims = (2, HALF, SEQUENCE_TOKENS)
    base = jnp.clip(jax.random.normal(key_rows[0], tensor_dims), -4.0, 4.0)
    return base.astype(jnp.float32)


def shard_levels(key, shape, cuts, low, largest):
    def one(position, parts):
        heights = jax.random.uniform(jax.random.fold_in(jax.random.fold_in(key, 6), position), (parts,), jnp.float32, low / len(cuts), largest / len(cuts))
        return jnp.repeat(jnp.exp(heights), shape[position] // parts).reshape((-1,) + (1,) * (len(shape) - position - 1))

    loudness = one(*cuts[0])
    for cut in cuts[1:]:
        loudness = loudness * one(*cut)
    return loudness


def bell_draw(key, shape, deviation, bound, cuts=(), kind=jnp.bfloat16):
    values = jax.random.normal(key, shape, jnp.float32) * deviation
    if len(cuts) > 0:
        values = shard_levels(key, shape, cuts, -0.22, 0.18) * values
    return jnp.clip(values, min=-bound, max=bound).astype(kind)


def setup_inputs(seed: int = 0, part: int = 0) -> dict:
    seeds = jax.random.split(jax.random.key(seed), 16)
    part_splits = jax.random.split(jax.random.fold_in(seeds[15], part), 16)
    return {
        "stream": bell_draw(part_splits[0], (SEQUENCE_TOKENS, D), 1.0, 6.0, ((0, 4),)),
        "queries_a": bell_draw(part_splits[1], (SEQUENCE_TOKENS, HALF * DKA), 1.0, 6.0, ((0, 4), (1, 4))),
        "keys_a": bell_draw(part_splits[2], (SEQUENCE_TOKENS, HALF * DKA), 1.0, 6.0, ((0, 4), (1, 4))),
        "queries_b": bell_draw(part_splits[3], (SEQUENCE_TOKENS, HALF * DKB), 1.0, 6.0, ((0, 4), (1, 4))),
        "keys_b": bell_draw(part_splits[4], (SEQUENCE_TOKENS, HALF * DKB), 1.0, 6.0, ((0, 4), (1, 4))),
        "values": bell_draw(part_splits[5], (SEQUENCE_TOKENS, 2, HALF * DV), 1.0, 6.0, ((0, 4), (2, 4))),
        "out_gate": bell_draw(part_splits[6], (SEQUENCE_TOKENS, 2, HALF * DV), 1.5, 6.0, ((0, 4), (2, 4))),
        "in_gate": draw_in_gate(jax.random.fold_in(jax.random.fold_in(seeds[15], part), 71), part),
        "forget_gate": draw_forget_gate(jax.random.fold_in(jax.random.fold_in(seeds[15], part), 71), part),
        "head_gain": jnp.clip(1.0 + 0.18 * jax.random.normal(seeds[9], (2, HALF * DV), jnp.float32), 0.1, 1.9),
        "out_weight": bell_draw(seeds[10], (2, HALF * DV, D), (2 * HALF * DV) ** -0.5, 0.125, ((1, 4),)),
        "norm_gain": jnp.clip(1.0 + 0.18 * jax.random.normal(seeds[11], (D,), jnp.float32), 0.1, 1.9),
        "gate_weight": bell_draw(seeds[12], (D, FF), D ** -0.5, 0.125, ((0, 4), (1, 4))),
        "up_weight": bell_draw(seeds[13], (D, FF), D ** -0.5, 0.125, ((0, 4), (1, 4))),
        "down_weight": bell_draw(seeds[14], (FF, D), FF ** -0.5, 0.078125, ((0, 4), (1, 4))),
    }


EPS = 1e-06
NEG = -1e+30
HIGHEST = lax.Precision.HIGHEST

def rounded(partial_value):
    return lax.optimization_barrier(partial_value.astype(jnp.bfloat16)).astype(jnp.float32)

def block_state(key_rows, values, in_rates, forget_rates):
    cumul = jnp.cumsum(jax.nn.log_sigmoid(forget_rates), axis=1)
    total = cumul[:, -1]
    tail = total[:, None] - cumul + in_rates
    peak = lax.optimization_barrier(jnp.max(tail, axis=1))
    weight = jnp.exp(tail - peak[:, None])
    weighted = rounded(values.astype(jnp.float32) * jnp.transpose(weight)[:, :, None])
    keys_wide = key_rows.astype(jnp.float32)
    state = jnp.einsum('rhv,rhk->hvk', weighted, keys_wide, precision=HIGHEST)
    norm_vec = jnp.einsum('hr,rhk->hk', weight, keys_wide, precision=HIGHEST)
    return ((state, norm_vec, peak, total), cumul)

def read_block(queries, key_rows, values, in_rates, cumul, carried, scale):
    length = queries.shape[0]
    query_wide = queries.astype(jnp.float32)
    scores = jnp.einsum('rhk,shk->hrs', query_wide, key_rows.astype(jnp.float32), precision=HIGHEST) * scale
    causal = lax.broadcasted_iota(jnp.int32, (length, length), 0) >= lax.broadcasted_iota(jnp.int32, (length, length), 1)
    decay_log = cumul[:, :, None] - cumul[:, None, :] + in_rates[:, None, :]
    decay_log = jnp.where(causal[None], decay_log, -jnp.inf)
    carried_log = cumul + carried[2][:, None]
    stabil = jnp.maximum(carried_log, lax.optimization_barrier(jnp.max(decay_log, axis=2)))
    weight_matrices = scores * jnp.exp(decay_log - stabil[:, :, None])
    carried_weight = jnp.exp(carried_log - stabil) * scale
    denom = lax.optimization_barrier(jnp.sum(weight_matrices, axis=2)) + carried_weight * jnp.einsum('hk,rhk->hr', carried[1], query_wide, precision=HIGHEST)
    numer = jnp.einsum('hrs,shv->rhv', rounded(weight_matrices), values.astype(jnp.float32), precision=HIGHEST)
    numer = numer + jnp.transpose(carried_weight)[:, :, None] * jnp.einsum('hvk,rhk->rhv', carried[0], query_wide, precision=HIGHEST)
    floor_val = jnp.maximum(jnp.abs(denom), jnp.exp(-stabil))
    return numer / jnp.transpose(floor_val)[:, :, None]

def combine_group(earlier, later):
    peak = jnp.maximum(later[3] + earlier[2], later[2])
    initial_scale = jnp.exp(later[3] + earlier[2] - peak)
    late_scale = jnp.exp(later[2] - peak)
    state = initial_scale[:, None, None] * earlier[0] + late_scale[:, None, None] * later[0]
    norm_vec = initial_scale[:, None] * earlier[1] + late_scale[:, None] * later[1]
    return (state, norm_vec, peak, earlier[3] + later[3])

def mixer_group(queries, key_rows, values, in_rates, forget_rates):
    key_size = queries.shape[1] // HALF
    blocks = SEQUENCE_TOKENS // TOK_DEV
    scale = key_size ** (-0.5)
    query_blocks = queries.reshape(blocks, TOK_DEV, HALF, key_size)
    key_blocks = key_rows.reshape(blocks, TOK_DEV, HALF, key_size)
    value_blocks = values.reshape(blocks, TOK_DEV, HALF, DV)
    in_blocks = jnp.transpose(in_rates.reshape(HALF, blocks, TOK_DEV), (1, 0, 2))
    forget_blocks = jnp.transpose(forget_rates.reshape(HALF, blocks, TOK_DEV), (1, 0, 2))

    def advance(carried, pieces):
        query_block, key_block, value_block, in_block, forget_block = pieces
        own, cumul = block_state(key_block, value_block, in_block, forget_block)
        cell = read_block(query_block, key_block, value_block, in_block, cumul, carried, scale)
        return (combine_group(carried, own), cell)
    start_state = (jnp.zeros((HALF, DV, key_size), jnp.float32), jnp.zeros((HALF, key_size), jnp.float32), jnp.full((HALF,), NEG, jnp.float32), jnp.zeros((HALF,), jnp.float32))
    _, cells = lax.scan(advance, start_state, (query_blocks, key_blocks, value_blocks, in_blocks, forget_blocks))
    return cells.reshape(SEQUENCE_TOKENS, HALF, DV)

def head_output(cell, gain, gate):
    lines = cell.shape[0]
    normed = cell * lax.rsqrt(lax.optimization_barrier(jnp.mean(cell * cell, axis=(1, 2), keepdims=True)) + EPS)
    return (normed.reshape(lines, -1) * gain * jax.nn.sigmoid(gate.astype(jnp.float32))).astype(jnp.bfloat16)

def reference(stream, queries_a, keys_a, queries_b, keys_b, values, out_gate, in_gate, forget_gate, head_gain, out_weight, norm_gain, gate_weight, up_weight, down_weight):
    mixed_first = head_output(mixer_group(queries_a, keys_a, values[:, 0], in_gate[0], forget_gate[0]), head_gain[0], out_gate[:, 0])
    mixed_second = head_output(mixer_group(queries_b, keys_b, values[:, 1], in_gate[1], forget_gate[1]), head_gain[1], out_gate[:, 1])
    width = HALF * DV // N_TP
    mixture = jnp.zeros((SEQUENCE_TOKENS, D), jnp.float32)
    for part_index in range(N_TP):
        cols = slice(part_index * width, (part_index + 1) * width)
        partial_value = jnp.dot(mixed_first[:, cols], out_weight[0, cols], preferred_element_type=jnp.float32)
        partial_value = partial_value + jnp.dot(mixed_second[:, cols], out_weight[1, cols], preferred_element_type=jnp.float32)
        mixture = mixture + rounded(partial_value)
    residual = stream.astype(jnp.float32) + mixture
    normed = (residual * lax.rsqrt(lax.optimization_barrier(jnp.mean(residual * residual, axis=1, keepdims=True)) + EPS) * norm_gain).astype(jnp.bfloat16)
    gate = jnp.dot(normed, gate_weight, preferred_element_type=jnp.float32)
    up_proj = jnp.dot(normed, up_weight, preferred_element_type=jnp.float32)
    active = (jax.nn.silu(gate) * up_proj).astype(jnp.bfloat16)
    hidden_part = FF // N_TP
    result = residual
    for part_index in range(N_TP):
        units = slice(part_index * hidden_part, (part_index + 1) * hidden_part)
        result = result + rounded(jnp.dot(active[:, units], down_weight[units], preferred_element_type=jnp.float32))
    return result.astype(jnp.bfloat16)
```

```python
import jax
import jax.numpy as jnp
from jax import lax
from jax.sharding import PartitionSpec as P

EPS = 1e-06
NEG = -1e30
HIGHEST = lax.Precision.HIGHEST


def entering(part, axis, combine, identity):
    size = lax.axis_size(axis)
    place = lax.axis_index(axis)
    width = part[0].shape[-1]
    bulk = [i for i, a in enumerate(part) if a.ndim == 3]
    small = [i for i, a in enumerate(part) if a.ndim < 3]
    flat = jnp.concatenate([part[i].reshape(-1) for i in small])
    flat = jnp.pad(flat, (0, -flat.shape[0] % width)).reshape(-1, width)
    packed = jnp.concatenate([part[i].reshape(-1, width) for i in bulk] + [flat])
    arrived = [
        lax.ppermute(packed, axis, [(i, i + shift) for i in range(size - shift)])
        for shift in range(1, size)
    ]
    state = tuple(jnp.asarray(e, a.dtype) for a, e in zip(part, identity))
    for shift in range(size - 1, 0, -1):
        block = arrived[shift - 1]
        later = [None] * len(part)
        row = 0
        for i in bulk:
            rows = part[i].size // width
            later[i] = block[row : row + rows].reshape(part[i].shape)
            row += rows
        rest = block[row:].reshape(-1)
        at = 0
        for i in small:
            later[i] = rest[at : at + part[i].size].reshape(part[i].shape)
            at += part[i].size
        present = place >= shift
        later = tuple(jnp.where(present, a, e) for a, e in zip(later, identity))
        state = combine(state, later)
    return state


def bits_of(axis):
    size = lax.axis_size(axis)
    return [1 << b for b in range(size.bit_length() - 1)]


def swap(value, axis, bit):
    return lax.ppermute(value, axis, [(i, i ^ bit) for i in range(lax.axis_size(axis))])


def gather_relative(own, axes_bits):
    held = own[None]
    for axis, bit in axes_bits:
        held = jnp.concatenate([held, swap(held, axis, bit)])
    return held


def scatter_sum_relative(blocks, axes_bits):
    held = blocks
    for axis, bit in reversed(axes_bits):
        half = held.shape[0] // 2
        other = swap(held[half:].astype(jnp.bfloat16), axis, bit)
        held = held[:half].astype(jnp.float32) + other.astype(jnp.float32)
    return held[0]


def block_state(key_rows, values, in_rates, forget_rates):
    cumul = jnp.cumsum(jax.nn.log_sigmoid(forget_rates), axis=1)
    total = cumul[:, -1]
    tail = total[:, None] - cumul + in_rates
    peak = jnp.max(tail, axis=1)
    weight = jnp.exp(tail - peak[:, None])
    weighted = (values.astype(jnp.float32) * jnp.transpose(weight)[:, :, None]).astype(jnp.bfloat16)
    state = jnp.einsum("rhk,rhv->hkv", key_rows, weighted, preferred_element_type=jnp.float32)
    norm_vec = jnp.einsum("hr,rhk->hk", weight, key_rows.astype(jnp.float32), precision=HIGHEST)
    return ((state, norm_vec, peak, total), cumul)


def read_block(queries, key_rows, values, in_rates, cumul, carried, scale):
    length = queries.shape[0]
    scores = (
        jnp.einsum("rhk,shk->hrs", queries, key_rows, preferred_element_type=jnp.float32) * scale
    )
    causal = lax.broadcasted_iota(jnp.int32, (length, length), 0) >= lax.broadcasted_iota(
        jnp.int32, (length, length), 1
    )
    decay_log = cumul[:, :, None] - cumul[:, None, :] + in_rates[:, None, :]
    decay_log = jnp.where(causal[None], decay_log, -jnp.inf)
    carried_log = cumul + carried[2][:, None]
    stabil = jnp.maximum(carried_log, jnp.max(decay_log, axis=2))
    weight_matrices = scores * jnp.exp(decay_log - stabil[:, :, None])
    carried_weight = jnp.exp(carried_log - stabil) * scale
    query_wide = queries.astype(jnp.float32)
    denom = jnp.sum(weight_matrices, axis=2) + carried_weight * jnp.einsum(
        "hk,rhk->hr", carried[1], query_wide, precision=HIGHEST
    )
    numer = jnp.einsum(
        "hrs,shv->rhv",
        weight_matrices.astype(jnp.bfloat16),
        values,
        preferred_element_type=jnp.float32,
    )
    numer = numer + jnp.transpose(carried_weight)[:, :, None] * jnp.einsum(
        "hkv,rhk->rhv", carried[0], query_wide, precision=HIGHEST
    )
    floor_val = jnp.maximum(jnp.abs(denom), jnp.exp(-stabil))
    return numer / jnp.transpose(floor_val)[:, :, None]


def combine_group(earlier, later):
    peak = jnp.maximum(later[3] + earlier[2], later[2])
    initial_scale = jnp.exp(later[3] + earlier[2] - peak)
    late_scale = jnp.exp(later[2] - peak)
    state = initial_scale[:, None, None] * earlier[0] + late_scale[:, None, None] * later[0]
    norm_vec = initial_scale[:, None] * earlier[1] + late_scale[:, None] * later[1]
    return (state, norm_vec, peak, earlier[3] + later[3])


def combine_both(earlier, later):
    return combine_group(earlier[:4], later[:4]) + combine_group(earlier[4:], later[4:])


def head_output(cell, mean_square, gain, gate):
    lines = cell.shape[0]
    normed = cell * lax.rsqrt(mean_square + EPS)[:, None, None]
    return (normed.reshape(lines, -1) * gain * jax.nn.sigmoid(gate.astype(jnp.float32))).astype(
        jnp.bfloat16
    )


def rms_normed(residual, gain):
    return (
        residual * lax.rsqrt(jnp.mean(residual * residual, axis=1, keepdims=True) + EPS) * gain
    ).astype(jnp.bfloat16)


def local(
    stream,
    queries_a,
    keys_a,
    queries_b,
    keys_b,
    values,
    out_gate,
    in_gate,
    forget_gate,
    head_gain,
    out_weight,
    norm_gain,
    gate_weight,
    up_weight,
    down_weight,
):
    parts = lax.axis_size("grp")
    hidden = gate_weight.shape[1] // parts
    first = lax.axis_index("grp") * hidden
    gate_whole, up_whole, down_whole = (
        lax.all_gather(
            lax.dynamic_slice_in_dim(gate_weight, first, hidden, 1), "sp", axis=0, tiled=True
        ),
        lax.all_gather(
            lax.dynamic_slice_in_dim(up_weight, first, hidden, 1), "sp", axis=0, tiled=True
        ),
        lax.all_gather(
            lax.dynamic_slice_in_dim(down_weight, first, hidden, 0), "sp", axis=1, tiled=True
        ),
    )
    length = stream.shape[0]
    heads = in_gate.shape[1]
    value_size = values.shape[2] // heads
    prepared = []
    own_states = []
    for group, (queries, key_rows) in enumerate(((queries_a, keys_a), (queries_b, keys_b))):
        key_size = queries.shape[1] // heads
        query_heads = queries.reshape(length, heads, key_size)
        key_heads = key_rows.reshape(length, heads, key_size)
        value_heads = values[:, group].reshape(length, heads, value_size)
        own, cumul = block_state(key_heads, value_heads, in_gate[group], forget_gate[group])
        own_states.append(own)
        prepared.append((query_heads, key_heads, value_heads, cumul, key_size))
    first_own, second_own = own_states
    size_first = prepared[0][4]
    size_second = prepared[1][4]
    carried = entering(
        (
            first_own[0],
            first_own[1],
            first_own[2],
            first_own[3],
            second_own[0],
            second_own[1],
            second_own[2],
            second_own[3],
        ),
        "sp",
        combine_both,
        (
            jnp.zeros((heads, size_first, value_size), jnp.float32),
            jnp.zeros((heads, size_first), jnp.float32),
            jnp.full((heads,), NEG, jnp.float32),
            jnp.zeros((heads,), jnp.float32),
            jnp.zeros((heads, size_second, value_size), jnp.float32),
            jnp.zeros((heads, size_second), jnp.float32),
            jnp.full((heads,), NEG, jnp.float32),
            jnp.zeros((heads,), jnp.float32),
        ),
    )
    cells = []
    for group in range(2):
        query_heads, key_heads, value_heads, cumul, key_size = prepared[group]
        cells.append(
            read_block(
                query_heads,
                key_heads,
                value_heads,
                in_gate[group],
                cumul,
                carried[4 * group : 4 * group + 3],
                key_size ** (-0.5),
            )
        )
    cell_first, cell_second = cells
    square_first = jnp.sum(cell_first * cell_first, axis=(1, 2))
    square_second = jnp.sum(cell_second * cell_second, axis=(1, 2))
    total_first, total_second = lax.psum((square_first, square_second), "tp")
    group_columns = heads * lax.axis_size("tp") * value_size
    mixed_first = head_output(cell_first, total_first / group_columns, head_gain[0], out_gate[:, 0])
    mixed_second = head_output(
        cell_second, total_second / group_columns, head_gain[1], out_gate[:, 1]
    )
    size = lax.axis_size("tp")
    share = length // size
    place = lax.axis_index("tp")
    tp_bits = [("tp", bit) for bit in reversed(bits_of("tp"))]
    order = [0]
    for _, bit in tp_bits:
        order = order + [p ^ bit for p in order]
    mixed = jnp.concatenate([mixed_first, mixed_second], axis=1)
    mixed = jnp.concatenate(
        [lax.dynamic_slice_in_dim(mixed, (place ^ p) * share, share, 0) for p in order]
    )
    width = mixed_first.shape[1]
    partial = (
        jnp.dot(mixed[:, :width], out_weight[0], preferred_element_type=jnp.float32)
        + jnp.dot(mixed[:, width:], out_weight[1], preferred_element_type=jnp.float32)
    ).astype(jnp.bfloat16)
    mixture = scatter_sum_relative(partial.reshape(size, share, -1), tp_bits)
    residual = lax.dynamic_slice_in_dim(stream, place * share, share, 0).astype(jnp.float32) + mixture
    both = [("grp", bit) for bit in bits_of("grp")] + tp_bits
    gathered = gather_relative(rms_normed(residual, norm_gain), both)
    count = gathered.shape[0]
    ffn_inputs = gathered.reshape(count * share, -1)
    gate = jnp.dot(ffn_inputs, gate_whole, preferred_element_type=jnp.float32)
    up_proj = jnp.dot(ffn_inputs, up_whole, preferred_element_type=jnp.float32)
    active = (jax.nn.silu(gate) * up_proj).astype(jnp.bfloat16)
    ffn_term = jnp.dot(active, down_whole, preferred_element_type=jnp.float32).astype(jnp.bfloat16)
    ffn_sum = scatter_sum_relative(ffn_term.reshape(count, share, -1), both)
    return (residual + ffn_sum).astype(jnp.bfloat16)


def solution(mesh):
    return jax.shard_map(
        local,
        mesh=mesh,
        in_specs=(
            P(("grp", "sp"), None),
            P(("grp", "sp"), "tp"),
            P(("grp", "sp"), "tp"),
            P(("grp", "sp"), "tp"),
            P(("grp", "sp"), "tp"),
            P(("grp", "sp"), None, "tp"),
            P(("grp", "sp"), None, "tp"),
            P(None, "tp", ("grp", "sp")),
            P(None, "tp", ("grp", "sp")),
            P(None, "tp"),
            P(None, "tp", None),
            P(),
            P("sp", "tp"),
            P("sp", "tp"),
            P("tp", "sp"),
        ),
        out_specs=P(("grp", "sp", "tp"), None),
        check_vma=False,
    )
```

```python
import jax
import jax.numpy as jnp
from jax import lax
from jax.sharding import PartitionSpec as P

EPS = 1e-06
NEG = -1e30
HIGHEST = lax.Precision.HIGHEST


def entering(part, axis, combine, identity):
    size = lax.axis_size(axis)
    place = lax.axis_index(axis)
    width = part[0].shape[-1]
    bulk = [i for i, a in enumerate(part) if a.ndim == 3]
    small = [i for i, a in enumerate(part) if a.ndim < 3]
    flat = jnp.concatenate([part[i].reshape(-1) for i in small])
    flat = jnp.pad(flat, (0, -flat.shape[0] % width)).reshape(-1, width)
    packed = jnp.concatenate([part[i].reshape(-1, width) for i in bulk] + [flat])
    arrived = [
        lax.ppermute(packed, axis, [(i, i + shift) for i in range(size - shift)])
        for shift in range(1, size)
    ]
    state = tuple(jnp.asarray(e, a.dtype) for a, e in zip(part, identity))
    for shift in range(size - 1, 0, -1):
        block = arrived[shift - 1]
        later = [None] * len(part)
        row = 0
        for i in bulk:
            rows = part[i].size // width
            later[i] = block[row : row + rows].reshape(part[i].shape)
            row += rows
        rest = block[row:].reshape(-1)
        at = 0
        for i in small:
            later[i] = rest[at : at + part[i].size].reshape(part[i].shape)
            at += part[i].size
        present = place >= shift
        later = tuple(jnp.where(present, a, e) for a, e in zip(later, identity))
        state = combine(state, later)
    return state


def bits_of(axis):
    size = lax.axis_size(axis)
    return [1 << b for b in range(size.bit_length() - 1)]


def swap(value, axis, bit):
    return lax.ppermute(value, axis, [(i, i ^ bit) for i in range(lax.axis_size(axis))])


def gather_relative(own, axes_bits):
    held = own[None]
    for axis, bit in axes_bits:
        held = jnp.concatenate([held, swap(held, axis, bit)])
    return held


def scatter_sum_relative(blocks, axes_bits):
    held = blocks
    for axis, bit in reversed(axes_bits):
        half = held.shape[0] // 2
        other = swap(held[half:].astype(jnp.bfloat16), axis, bit)
        held = held[:half].astype(jnp.float32) + other.astype(jnp.float32)
    return held[0]


def scatter_sum_ordered(blocks, stages):
    held = blocks.reshape((2,) * len(stages) + blocks.shape[1:])
    for dimension, (axis, bit) in stages:
        kept = lax.slice_in_dim(held, 0, 1, axis=dimension)
        sent = lax.slice_in_dim(held, 1, 2, axis=dimension)
        other = swap(sent.astype(jnp.bfloat16), axis, bit)
        held = kept.astype(jnp.float32) + other.astype(jnp.float32)
    return held.reshape(blocks.shape[1:])


def block_state(key_rows, values, in_rates, forget_rates):
    cumul = jnp.cumsum(jax.nn.log_sigmoid(forget_rates), axis=1)
    total = cumul[:, -1]
    tail = total[:, None] - cumul + in_rates
    peak = jnp.max(tail, axis=1)
    weight = jnp.exp(tail - peak[:, None])
    weighted = (values.astype(jnp.float32) * jnp.transpose(weight)[:, :, None]).astype(jnp.bfloat16)
    state = jnp.einsum("rhk,rhv->hkv", key_rows, weighted, preferred_element_type=jnp.float32)
    norm_vec = jnp.einsum("hr,rhk->hk", weight, key_rows.astype(jnp.float32), precision=HIGHEST)
    return ((state, norm_vec, peak, total), cumul)


def read_block(queries, key_rows, values, in_rates, cumul, carried, scale):
    length = queries.shape[0]
    scores = (
        jnp.einsum("rhk,shk->hrs", queries, key_rows, preferred_element_type=jnp.float32) * scale
    )
    causal = lax.broadcasted_iota(jnp.int32, (length, length), 0) >= lax.broadcasted_iota(
        jnp.int32, (length, length), 1
    )
    decay_log = cumul[:, :, None] - cumul[:, None, :] + in_rates[:, None, :]
    decay_log = jnp.where(causal[None], decay_log, -jnp.inf)
    carried_log = cumul + carried[2][:, None]
    stabil = jnp.maximum(carried_log, jnp.max(decay_log, axis=2))
    weight_matrices = scores * jnp.exp(decay_log - stabil[:, :, None])
    carried_weight = jnp.exp(carried_log - stabil) * scale
    query_wide = queries.astype(jnp.float32)
    denom = jnp.sum(weight_matrices, axis=2) + carried_weight * jnp.einsum(
        "hk,rhk->hr", carried[1], query_wide, precision=HIGHEST
    )
    numer = jnp.einsum(
        "hrs,shv->rhv",
        weight_matrices.astype(jnp.bfloat16),
        values,
        preferred_element_type=jnp.float32,
    )
    numer = numer + jnp.transpose(carried_weight)[:, :, None] * jnp.einsum(
        "hkv,rhk->rhv", carried[0], query_wide, precision=HIGHEST
    )
    floor_val = jnp.maximum(jnp.abs(denom), jnp.exp(-stabil))
    return numer / jnp.transpose(floor_val)[:, :, None]


def combine_group(earlier, later):
    peak = jnp.maximum(later[3] + earlier[2], later[2])
    initial_scale = jnp.exp(later[3] + earlier[2] - peak)
    late_scale = jnp.exp(later[2] - peak)
    state = initial_scale[:, None, None] * earlier[0] + late_scale[:, None, None] * later[0]
    norm_vec = initial_scale[:, None] * earlier[1] + late_scale[:, None] * later[1]
    return (state, norm_vec, peak, earlier[3] + later[3])


def combine_both(earlier, later):
    return combine_group(earlier[:4], later[:4]) + combine_group(earlier[4:], later[4:])


def head_output(cell, mean_square, gain, gate):
    lines = cell.shape[0]
    normed = cell * lax.rsqrt(mean_square + EPS)[:, None, None]
    return (normed.reshape(lines, -1) * gain * jax.nn.sigmoid(gate.astype(jnp.float32))).astype(
        jnp.bfloat16
    )


def rms_normed(residual, gain):
    return (
        residual * lax.rsqrt(jnp.mean(residual * residual, axis=1, keepdims=True) + EPS) * gain
    ).astype(jnp.bfloat16)


def local(
    stream,
    queries_a,
    keys_a,
    queries_b,
    keys_b,
    values,
    out_gate,
    in_gate,
    forget_gate,
    head_gain,
    out_weight,
    norm_gain,
    gate_weight,
    up_weight,
    down_weight,
):
    parts = lax.axis_size("grp")
    hidden = gate_weight.shape[1] // parts
    first = lax.axis_index("grp") * hidden
    gate_up_whole = lax.all_gather(
        jnp.stack(
            [
                lax.dynamic_slice_in_dim(gate_weight, first, hidden, 1),
                lax.dynamic_slice_in_dim(up_weight, first, hidden, 1),
            ]
        ),
        "sp",
        axis=1,
        tiled=True,
    )
    down_whole = lax.all_gather(
        lax.dynamic_slice_in_dim(down_weight, first, hidden, 0), "sp", axis=1, tiled=True
    )
    length = stream.shape[0]
    heads = in_gate.shape[1]
    value_size = values.shape[2] // heads
    prepared = []
    own_states = []
    for group, (queries, key_rows) in enumerate(((queries_a, keys_a), (queries_b, keys_b))):
        key_size = queries.shape[1] // heads
        query_heads = queries.reshape(length, heads, key_size)
        key_heads = key_rows.reshape(length, heads, key_size)
        value_heads = values[:, group].reshape(length, heads, value_size)
        own, cumul = block_state(key_heads, value_heads, in_gate[group], forget_gate[group])
        own_states.append(own)
        prepared.append((query_heads, key_heads, value_heads, cumul, key_size))
    first_own, second_own = own_states
    size_first = prepared[0][4]
    size_second = prepared[1][4]
    carried = entering(
        (
            first_own[0],
            first_own[1],
            first_own[2],
            first_own[3],
            second_own[0],
            second_own[1],
            second_own[2],
            second_own[3],
        ),
        "sp",
        combine_both,
        (
            jnp.zeros((heads, size_first, value_size), jnp.float32),
            jnp.zeros((heads, size_first), jnp.float32),
            jnp.full((heads,), NEG, jnp.float32),
            jnp.zeros((heads,), jnp.float32),
            jnp.zeros((heads, size_second, value_size), jnp.float32),
            jnp.zeros((heads, size_second), jnp.float32),
            jnp.full((heads,), NEG, jnp.float32),
            jnp.zeros((heads,), jnp.float32),
        ),
    )
    cells = []
    for group in range(2):
        query_heads, key_heads, value_heads, cumul, key_size = prepared[group]
        cells.append(
            read_block(
                query_heads,
                key_heads,
                value_heads,
                in_gate[group],
                cumul,
                carried[4 * group : 4 * group + 3],
                key_size ** (-0.5),
            )
        )
    cell_first, cell_second = cells
    square_first = jnp.sum(cell_first * cell_first, axis=(1, 2))
    square_second = jnp.sum(cell_second * cell_second, axis=(1, 2))
    total_first, total_second = lax.psum((square_first, square_second), "tp")
    group_columns = heads * lax.axis_size("tp") * value_size
    mixed_first = head_output(cell_first, total_first / group_columns, head_gain[0], out_gate[:, 0])
    mixed_second = head_output(
        cell_second, total_second / group_columns, head_gain[1], out_gate[:, 1]
    )
    size = lax.axis_size("tp")
    share = length // size
    place = lax.axis_index("tp")
    tp_bits = [("tp", bit) for bit in reversed(bits_of("tp"))]
    order = [0]
    for _, bit in tp_bits:
        order = order + [p ^ bit for p in order]
    mixed = jnp.concatenate([mixed_first, mixed_second], axis=1)
    mixed = jnp.concatenate(
        [lax.dynamic_slice_in_dim(mixed, (place ^ p) * share, share, 0) for p in order]
    )
    width = mixed_first.shape[1]
    partial = (
        jnp.dot(mixed[:, :width], out_weight[0], preferred_element_type=jnp.float32)
        + jnp.dot(mixed[:, width:], out_weight[1], preferred_element_type=jnp.float32)
    ).astype(jnp.bfloat16)
    mixture = scatter_sum_relative(partial.reshape(size, share, -1), tp_bits)
    residual = lax.dynamic_slice_in_dim(stream, place * share, share, 0).astype(jnp.float32) + mixture
    both = [("grp", bit) for bit in bits_of("grp")] + tp_bits
    gathered = gather_relative(rms_normed(residual, norm_gain), both)
    count = gathered.shape[0]
    ffn_inputs = gathered.reshape(count * share, -1)
    gate = jnp.dot(ffn_inputs, gate_up_whole[0], preferred_element_type=jnp.float32)
    up_proj = jnp.dot(ffn_inputs, gate_up_whole[1], preferred_element_type=jnp.float32)
    active = (jax.nn.silu(gate) * up_proj).astype(jnp.bfloat16)
    chunks = max(len(both) - 1, 1)
    columns = down_whole.shape[1] // chunks
    stages = list(enumerate(reversed(both)))
    sums = []
    for chunk in range(chunks):
        term = jnp.dot(
            active,
            down_whole[:, chunk * columns : (chunk + 1) * columns],
            preferred_element_type=jnp.float32,
        ).astype(jnp.bfloat16)
        late = stages[1:]
        late = late[chunk:] + late[:chunk]
        sums.append(scatter_sum_ordered(term.reshape(count, share, columns), stages[:1] + late))
    ffn_sum = jnp.concatenate(sums, axis=1)
    return (residual + ffn_sum).astype(jnp.bfloat16)


def solution(mesh):
    return jax.shard_map(
        local,
        mesh=mesh,
        in_specs=(
            P(("grp", "sp"), None),
            P(("grp", "sp"), "tp"),
            P(("grp", "sp"), "tp"),
            P(("grp", "sp"), "tp"),
            P(("grp", "sp"), "tp"),
            P(("grp", "sp"), None, "tp"),
            P(("grp", "sp"), None, "tp"),
            P(None, "tp", ("grp", "sp")),
            P(None, "tp", ("grp", "sp")),
            P(None, "tp"),
            P(None, "tp", None),
            P(),
            P("sp", "tp"),
            P("sp", "tp"),
            P("tp", "sp"),
        ),
        out_specs=P(("grp", "sp", "tp"), None),
        check_vma=False,
    )
```

```python
import jax
import jax.numpy as jnp
from jax import lax
from jax.sharding import PartitionSpec as P

EPS = 1e-06
NEG = -1e30
HIGHEST = lax.Precision.HIGHEST


def entering(part, axis, combine, identity):
    size = lax.axis_size(axis)
    place = lax.axis_index(axis)
    width = part[0].shape[-1]
    bulk = [i for i, a in enumerate(part) if a.ndim == 3]
    small = [i for i, a in enumerate(part) if a.ndim < 3]
    flat = jnp.concatenate([part[i].reshape(-1) for i in small])
    flat = jnp.pad(flat, (0, -flat.shape[0] % width)).reshape(-1, width)
    packed = jnp.concatenate([part[i].reshape(-1, width) for i in bulk] + [flat])
    arrived = [
        lax.ppermute(packed, axis, [(i, i + shift) for i in range(size - shift)])
        for shift in range(1, size)
    ]
    state = tuple(jnp.asarray(e, a.dtype) for a, e in zip(part, identity))
    for shift in range(size - 1, 0, -1):
        block = arrived[shift - 1]
        later = [None] * len(part)
        row = 0
        for i in bulk:
            rows = part[i].size // width
            later[i] = block[row : row + rows].reshape(part[i].shape)
            row += rows
        rest = block[row:].reshape(-1)
        at = 0
        for i in small:
            later[i] = rest[at : at + part[i].size].reshape(part[i].shape)
            at += part[i].size
        present = place >= shift
        later = tuple(jnp.where(present, a, e) for a, e in zip(later, identity))
        state = combine(state, later)
    return state


def moved(block, pairs):
    return lax.ppermute(block, "sp", pairs)


def bits_of(axis):
    size = lax.axis_size(axis)
    return [1 << b for b in range(size.bit_length() - 1)]


def swap(value, axis, bit):
    return lax.ppermute(value, axis, [(i, i ^ bit) for i in range(lax.axis_size(axis))])


def gather_relative(own, axes_bits):
    held = own[None]
    for axis, bit in axes_bits:
        held = jnp.concatenate([held, swap(held, axis, bit)])
    return held


def scatter_sum_relative(blocks, axes_bits):
    held = blocks
    for axis, bit in reversed(axes_bits):
        half = held.shape[0] // 2
        other = swap(held[half:].astype(jnp.bfloat16), axis, bit)
        held = held[:half].astype(jnp.float32) + other.astype(jnp.float32)
    return held[0]


def scatter_sum_ordered(blocks, stages):
    held = blocks.reshape((2,) * len(stages) + blocks.shape[1:])
    for dimension, (axis, bit) in stages:
        kept = lax.slice_in_dim(held, 0, 1, axis=dimension)
        sent = lax.slice_in_dim(held, 1, 2, axis=dimension)
        other = swap(sent.astype(jnp.bfloat16), axis, bit)
        held = kept.astype(jnp.float32) + other.astype(jnp.float32)
    return held.reshape(blocks.shape[1:])


def block_state(key_rows, values, in_rates, forget_rates):
    cumul = jnp.cumsum(jax.nn.log_sigmoid(forget_rates), axis=1)
    total = cumul[:, -1]
    tail = total[:, None] - cumul + in_rates
    peak = jnp.max(tail, axis=1)
    weight = jnp.exp(tail - peak[:, None])
    weighted = (values.astype(jnp.float32) * jnp.transpose(weight)[:, :, None]).astype(jnp.bfloat16)
    state = jnp.einsum("rhk,rhv->hkv", key_rows, weighted, preferred_element_type=jnp.float32)
    norm_vec = jnp.einsum("hr,rhk->hk", weight, key_rows.astype(jnp.float32), precision=HIGHEST)
    return ((state, norm_vec, peak, total), cumul)


def read_block(queries, key_rows, values, in_rates, cumul, carried, scale):
    length = queries.shape[0]
    scores = (
        jnp.einsum("rhk,shk->hrs", queries, key_rows, preferred_element_type=jnp.float32) * scale
    )
    causal = lax.broadcasted_iota(jnp.int32, (length, length), 0) >= lax.broadcasted_iota(
        jnp.int32, (length, length), 1
    )
    decay_log = cumul[:, :, None] - cumul[:, None, :] + in_rates[:, None, :]
    decay_log = jnp.where(causal[None], decay_log, -jnp.inf)
    carried_log = cumul + carried[2][:, None]
    stabil = jnp.maximum(carried_log, jnp.max(decay_log, axis=2))
    weight_matrices = scores * jnp.exp(decay_log - stabil[:, :, None])
    carried_weight = jnp.exp(carried_log - stabil) * scale
    query_wide = queries.astype(jnp.float32)
    denom = jnp.sum(weight_matrices, axis=2) + carried_weight * jnp.einsum(
        "hk,rhk->hr", carried[1], query_wide, precision=HIGHEST
    )
    numer = jnp.einsum(
        "hrs,shv->rhv",
        weight_matrices.astype(jnp.bfloat16),
        values,
        preferred_element_type=jnp.float32,
    )
    numer = numer + jnp.transpose(carried_weight)[:, :, None] * jnp.einsum(
        "hkv,rhk->rhv", carried[0], query_wide, precision=HIGHEST
    )
    floor_val = jnp.maximum(jnp.abs(denom), jnp.exp(-stabil))
    return numer / jnp.transpose(floor_val)[:, :, None]


def combine_group(earlier, later):
    peak = jnp.maximum(later[3] + earlier[2], later[2])
    initial_scale = jnp.exp(later[3] + earlier[2] - peak)
    late_scale = jnp.exp(later[2] - peak)
    state = initial_scale[:, None, None] * earlier[0] + late_scale[:, None, None] * later[0]
    norm_vec = initial_scale[:, None] * earlier[1] + late_scale[:, None] * later[1]
    return (state, norm_vec, peak, earlier[3] + later[3])


def combine_both(earlier, later):
    return combine_group(earlier[:4], later[:4]) + combine_group(earlier[4:], later[4:])


def head_output(cell, mean_square, gain, gate):
    lines = cell.shape[0]
    normed = cell * lax.rsqrt(mean_square + EPS)[:, None, None]
    return (normed.reshape(lines, -1) * gain * jax.nn.sigmoid(gate.astype(jnp.float32))).astype(
        jnp.bfloat16
    )


def rms_normed(residual, gain):
    return (
        residual * lax.rsqrt(jnp.mean(residual * residual, axis=1, keepdims=True) + EPS) * gain
    ).astype(jnp.bfloat16)


def local(
    stream,
    queries_a,
    keys_a,
    queries_b,
    keys_b,
    values,
    out_gate,
    in_gate,
    forget_gate,
    head_gain,
    out_weight,
    norm_gain,
    gate_weight,
    up_weight,
    down_weight,
):
    parts = lax.axis_size("grp")
    hidden = gate_weight.shape[1] // parts
    first = lax.axis_index("grp") * hidden
    gate_up_whole = lax.all_gather(
        jnp.stack(
            [
                lax.dynamic_slice_in_dim(gate_weight, first, hidden, 1),
                lax.dynamic_slice_in_dim(up_weight, first, hidden, 1),
            ]
        ),
        "sp",
        axis=1,
        tiled=True,
    )
    down = lax.dynamic_slice_in_dim(down_weight, first, hidden, 0)
    length = stream.shape[0]
    heads = in_gate.shape[1]
    value_size = values.shape[2] // heads
    prepared = []
    own_states = []
    for group, (queries, key_rows) in enumerate(((queries_a, keys_a), (queries_b, keys_b))):
        key_size = queries.shape[1] // heads
        query_heads = queries.reshape(length, heads, key_size)
        key_heads = key_rows.reshape(length, heads, key_size)
        value_heads = values[:, group].reshape(length, heads, value_size)
        own, cumul = block_state(key_heads, value_heads, in_gate[group], forget_gate[group])
        own_states.append(own)
        prepared.append((query_heads, key_heads, value_heads, cumul, key_size))
    first_own, second_own = own_states
    size_first = prepared[0][4]
    size_second = prepared[1][4]
    carried = entering(
        (
            first_own[0],
            first_own[1],
            first_own[2],
            first_own[3],
            second_own[0],
            second_own[1],
            second_own[2],
            second_own[3],
        ),
        "sp",
        combine_both,
        (
            jnp.zeros((heads, size_first, value_size), jnp.float32),
            jnp.zeros((heads, size_first), jnp.float32),
            jnp.full((heads,), NEG, jnp.float32),
            jnp.zeros((heads,), jnp.float32),
            jnp.zeros((heads, size_second, value_size), jnp.float32),
            jnp.zeros((heads, size_second), jnp.float32),
            jnp.full((heads,), NEG, jnp.float32),
            jnp.zeros((heads,), jnp.float32),
        ),
    )
    down, carried = lax.optimization_barrier((down, carried))
    ring = lax.axis_size("sp")
    blocks = [down] + [
        moved(down, [((i + ahead) % ring, i) for i in range(ring)])
        for ahead in range(1, ring)
    ]
    cells = []
    for group in range(2):
        query_heads, key_heads, value_heads, cumul, key_size = prepared[group]
        cells.append(
            read_block(
                query_heads,
                key_heads,
                value_heads,
                in_gate[group],
                cumul,
                carried[4 * group : 4 * group + 3],
                key_size ** (-0.5),
            )
        )
    cell_first, cell_second = cells
    square_first = jnp.sum(cell_first * cell_first, axis=(1, 2))
    square_second = jnp.sum(cell_second * cell_second, axis=(1, 2))
    total_first, total_second = lax.psum((square_first, square_second), "tp")
    group_columns = heads * lax.axis_size("tp") * value_size
    mixed_first = head_output(cell_first, total_first / group_columns, head_gain[0], out_gate[:, 0])
    mixed_second = head_output(
        cell_second, total_second / group_columns, head_gain[1], out_gate[:, 1]
    )
    size = lax.axis_size("tp")
    share = length // size
    place = lax.axis_index("tp")
    tp_bits = [("tp", bit) for bit in reversed(bits_of("tp"))]
    order = [0]
    for _, bit in tp_bits:
        order = order + [p ^ bit for p in order]
    mixed = jnp.concatenate([mixed_first, mixed_second], axis=1)
    mixed = jnp.concatenate(
        [lax.dynamic_slice_in_dim(mixed, (place ^ p) * share, share, 0) for p in order]
    )
    width = mixed_first.shape[1]
    partial = (
        jnp.dot(mixed[:, :width], out_weight[0], preferred_element_type=jnp.float32)
        + jnp.dot(mixed[:, width:], out_weight[1], preferred_element_type=jnp.float32)
    ).astype(jnp.bfloat16)
    mixture = scatter_sum_relative(partial.reshape(size, share, -1), tp_bits)
    residual = lax.dynamic_slice_in_dim(stream, place * share, share, 0).astype(jnp.float32) + mixture
    both = [("grp", bit) for bit in bits_of("grp")] + tp_bits
    gathered = gather_relative(rms_normed(residual, norm_gain), both)
    count = gathered.shape[0]
    ffn_inputs = gathered.reshape(count * share, -1)
    gate = jnp.dot(ffn_inputs, gate_up_whole[0], preferred_element_type=jnp.float32)
    up_proj = jnp.dot(ffn_inputs, gate_up_whole[1], preferred_element_type=jnp.float32)
    active = (jax.nn.silu(gate) * up_proj).astype(jnp.bfloat16)
    down_whole = lax.dynamic_slice_in_dim(
        jnp.concatenate(blocks + blocks, axis=1),
        (ring - lax.axis_index("sp")) * down.shape[1],
        ring * down.shape[1],
        1,
    )
    chunks = max(len(both) - 1, 1)
    columns = down_whole.shape[1] // chunks
    stages = list(enumerate(reversed(both)))
    sums = []
    for chunk in range(chunks):
        term = jnp.dot(
            active,
            down_whole[:, chunk * columns : (chunk + 1) * columns],
            preferred_element_type=jnp.float32,
        ).astype(jnp.bfloat16)
        late = stages[1:]
        late = late[chunk:] + late[:chunk]
        sums.append(scatter_sum_ordered(term.reshape(count, share, columns), stages[:1] + late))
    ffn_sum = jnp.concatenate(sums, axis=1)
    return (residual + ffn_sum).astype(jnp.bfloat16)


def solution(mesh):
    return jax.shard_map(
        local,
        mesh=mesh,
        in_specs=(
            P(("grp", "sp"), None),
            P(("grp", "sp"), "tp"),
            P(("grp", "sp"), "tp"),
            P(("grp", "sp"), "tp"),
            P(("grp", "sp"), "tp"),
            P(("grp", "sp"), None, "tp"),
            P(("grp", "sp"), None, "tp"),
            P(None, "tp", ("grp", "sp")),
            P(None, "tp", ("grp", "sp")),
            P(None, "tp"),
            P(None, "tp", None),
            P(),
            P("sp", "tp"),
            P("sp", "tp"),
            P("tp", "sp"),
        ),
        out_specs=P(("grp", "sp", "tp"), None),
        check_vma=False,
    )
```
